256 devices in a mesh: sp: 64 (over z, x, core), tp: 4 (over y).
Axes of the slice: x: 4, y: 4, z: 8, core: 2. Of those that a mesh axis runs over, the one named last changes fastest.
Arguments:
- out_cotangent: bfloat16 [16384, 2048], P('sp'), may hold values from -16 to 16
- stream: bfloat16 [16384, 2048], P('sp'), may hold values from -6 to 6
- route_ids: int32 [16384, 2], P('sp'), may hold values from 0 to 63, all different within a row; in each aligned block of 256 rows (0 to 255, 256 to 511, ...) at most 16 rows name the same one
- route_weights: float32 [16384, 2], P('sp'), may hold values from 0.3 to 2
- gate_proj: bfloat16 [64, 2048, 1024], P('sp', None, 'tp'), may hold values from -0.125 to 0.125
- up_proj: bfloat16 [64, 2048, 1024], P('sp', None, 'tp'), may hold values from -0.125 to 0.125
- down_proj: bfloat16 [64, 1024, 2048], P('sp', 'tp'), may hold values from -0.1875 to 0.1875
- outer_gate: bfloat16 [16384, 512], P('sp', 'tp'), may hold values from -6 to 6
- inner_gate: bfloat16 [16384, 512], P('sp', 'tp'), may hold values from -6 to 6
- conv_input: bfloat16 [16384, 512], P('sp', 'tp'), may hold values from -6 to 6
- conv_taps: float32 [3, 512], P(None, 'tp'), may hold values from -4 to 4
- out_proj: bfloat16 [2048, 512], P(None, 'tp'), may hold values from -0.25 to 0.25
Outputs:
- grad_gate_proj: bfloat16 [64, 2048, 1024], P('sp', None, 'tp')
- grad_up_proj: bfloat16 [64, 2048, 1024], P('sp', None, 'tp')
- grad_down_proj: bfloat16 [64, 1024, 2048], P('sp', 'tp')
- grad_out_proj: float32 [2048, 512], P('sp', 'tp')
- grad_outer_gate: float32 [16384, 512], P('sp', 'tp')
- grad_inner_gate: float32 [16384, 512], P('sp', 'tp')
- grad_conv_input: float32 [16384, 512], P('sp', 'tp')
The draws below stay inside these ranges and needn't reach their ends.
Inputs may be any that keep to these rules, and one draw needn't show every extreme that they name: `route_ids`: the 2 experts of a token differ. Among the tokens of one index of sp, no expert is chosen more than 16 times, and in every draw some expert is chosen exactly 16 times by them.
All inputs are finite; a program needn't handle non-finite values.
Results may differ from the reference program's by a relative error of at most 0.018.
Values may be sent and summed in bfloat16 or wider, within the bound.
No kernel may reach another device: no remote copies, remote signals or barrier semaphores. Data moves between devices by JAX's collectives and lax.ppermute only.
A program may use at most 64 MiB of HBM per device.

```python
import math
import jax
import jax.numpy as jnp
import numpy as np
from jax import lax

D = 2048
FF = 1024
CONV = 512
TAPS = 3
TOPK = 2
TOK_DEV = 256
EXPERTS = 64
CAP = 16
SLOTS = 1024
TOKENS = 16384
N_TP = 4


def with_spikes(entries, rng, source, target, shards_of, factor):
    owner, partner = [(jnp.arange(entries.shape[dim]) // (entries.shape[dim] // shards_of)).reshape([-1 if axis == dim else 1 for axis in range(entries.ndim)]) for dim in (source, target)]
    chosen = jax.random.permutation(rng, shards_of)[partner]
    strong = (owner == chosen) | (owner == (partner + shards_of // 2) % shards_of)
    return jnp.where(strong, factor * entries, entries)


def block_levels(stream_key, dims, cuts, low, largest):
    def one(dim, parts):
        heights = jax.random.uniform(jax.random.fold_in(jax.random.fold_in(stream_key, 6), dim), (parts,), jnp.float32, low / len(cuts), largest / len(cuts))
        return jnp.repeat(jnp.exp(heights), dims[dim] // parts).reshape((-1,) + (1,) * (len(dims) - dim - 1))

    gain = one(*cuts[0])
    for cut in cuts[1:]:
        gain = gain * one(*cut)
    return gain


def deal_out(own_key, own, number, rows, count, top, reach, lean):
    sequence = jax.random.permutation(own_key, count)
    heavy_load, ordinary = shares(count, rows * top, reach, lean, True), shares(count, rows * top, reach, lean, False)
    places = jnp.arange(count)

    def named(tallies, turn):
        used = int((tallies > 0).sum())
        fixed = max(1, used // 4)
        moved = fixed + (places - fixed + turn * (used - fixed)) % max(1, count - fixed)
        return jnp.zeros((count,), jnp.int32).at[sequence[jnp.where(places < fixed, places, moved)]].set(jnp.asarray(tallies, jnp.int32))

    tallies = jnp.where(number % 4 == 0, named(heavy_load, number // 4), named(ordinary, number - number // 4 - 1))
    mixed = jax.random.permutation(jax.random.fold_in(own, 3), count)
    donor, sink = mixed[0:count // 2 * 2:2], mixed[1:count // 2 * 2:2]
    room = jnp.minimum(tallies[donor] - 1, reach - tallies[sink]) // 2
    room = jnp.where((donor == sequence[0]) | (sink == sequence[0]) | (tallies[sink] == 0), 0, jnp.maximum(room, 0))
    moved = jax.random.randint(jax.random.fold_in(own, 4), (count // 2,), 0, 1 << 20) % (room + 1)
    tallies = tallies.at[donor].add(-moved).at[sink].add(moved)
    labels = jnp.searchsorted(jnp.cumsum(tallies), jnp.arange(rows * top), side="right").astype(jnp.int32)
    table = labels.reshape(top, rows).T
    table = table[jax.random.permutation(jax.random.fold_in(own, 1), rows)]
    turn = jax.random.randint(jax.random.fold_in(own, 2), (rows, 1), 0, top)
    return jnp.take_along_axis(table, (jnp.arange(top)[None, :] + turn) % top, axis=1)


def shares(number_of, total, reach, skew, full):
    portions = [(1 << 20) // math.isqrt(grade ** skew) + 1 for grade in range(1, number_of + 1)]
    largest = reach if full else min(reach, max(-(-total // number_of), total * portions[0] // sum(portions)))
    least = 1 if total - largest >= number_of - 1 else 0
    counts, rest = [largest] + [least] * (number_of - 1), total - largest - least * (number_of - 1)
    while rest > 0:
        movable = [i for i in range(1, number_of) if counts[i] < largest] or [i for i in range(1, number_of) if counts[i] < reach]
        whole, left = sum([portions[i] for i in movable]), rest
        for i in movable:
            more = min(reach - counts[i], max(1, left * portions[i] // whole), rest)
            counts[i] = counts[i] + more
            rest = rest - more
    return np.array(counts)


def bell_draw(own_key, dims, deviation, bound, cuts=(), kind=jnp.bfloat16):
    loudness = block_levels(own_key, dims, cuts, -0.22, 0.18) if cuts else 1.0
    entries = jax.random.normal(own_key, dims, jnp.float32) * deviation * loudness
    return jnp.minimum(jnp.maximum(entries, -bound), bound).astype(kind)


def bell_draw_with(stream_key, extent, width, most, cuts, heavy, kind=jnp.bfloat16):
    values = width * jax.random.normal(stream_key, extent, jnp.float32)
    if cuts:
        values = values * block_levels(stream_key, extent, cuts, -0.22, 0.18)
    return jnp.clip(with_spikes(values, jax.random.fold_in(stream_key, 3), *heavy), -most, most).astype(kind)


def setup_inputs(seed: int = 0) -> dict:
    seeds = jax.random.split(jax.random.key(seed), 13)
    out_cotangent = bell_draw_with(seeds[0], (TOKENS, D), 1.0, 16.0, ((0, 64),), (0, 1, 64, 4.0))
    stream = bell_draw(seeds[1], (TOKENS, D), 1.0, 6.0, ((0, 64),))
    route_ids_keys = jax.random.split(jax.random.fold_in(seeds[2], 1), TOKENS // TOK_DEV)
    route_ids_turns = jax.random.permutation(jax.random.fold_in(seeds[2], 3), TOKENS // TOK_DEV)
    route_ids = jax.vmap(lambda own, number: deal_out(jax.random.fold_in(seeds[2], 2), own, number, TOK_DEV, EXPERTS, TOPK, CAP, 1))(route_ids_keys, route_ids_turns).reshape((TOKENS, TOPK))
    route_weights = jnp.clip(0.3 + 1.7 * jax.random.uniform(seeds[3], (TOKENS, TOPK), jnp.float32) ** block_levels(seeds[3], (TOKENS, TOPK), ((0, 64),), -0.2, 0.2), 0.3, 2.0)
    gate_proj = bell_draw(seeds[4], (EXPERTS, D, FF), D ** -0.5, 0.125, ((0, 64), (2, 4)))
    up_proj = bell_draw(seeds[5], (EXPERTS, D, FF), D ** -0.5, 0.125, ((0, 64), (2, 4)))
    down_proj = bell_draw(seeds[6], (EXPERTS, FF, D), FF ** -0.5, 0.1875, ((0, 64), (1, 4)))
    outer_gate = bell_draw(seeds[7], (TOKENS, CONV), 1.0, 6.0, ((0, 64), (1, 4)))
    inner_gate = bell_draw(seeds[8], (TOKENS, CONV), 1.0, 6.0, ((0, 64), (1, 4)))
    conv_input = bell_draw(seeds[9], (TOKENS, CONV), 1.0, 6.0, ((0, 64), (1, 4)))
    conv_taps = bell_draw(seeds[10], (TAPS, CONV), 0.6, 4.0, ((1, 4),), jnp.float32)
    out_proj = bell_draw(seeds[11], (D, CONV), CONV ** -0.5, 0.25, ((1, 4),))
    return dict(out_cotangent=out_cotangent, stream=stream, route_ids=route_ids, route_weights=route_weights, gate_proj=gate_proj, up_proj=up_proj, down_proj=down_proj, outer_gate=outer_gate, inner_gate=inner_gate, conv_input=conv_input, conv_taps=conv_taps, out_proj=out_proj)


def expert_backward(out_cotangent, stream, route_ids, route_weights, w_gate, w_up, w_down, expert):
    chosen = route_ids == expert
    weight = jnp.sum(jnp.where(chosen, route_weights, 0.0), axis=1)
    hit = jnp.any(chosen, axis=1)
    index = jnp.nonzero(hit, size=SLOTS, fill_value=0)[0].astype(jnp.int32)
    count = jnp.sum(hit.astype(jnp.int32))
    valid = jnp.arange(SLOTS, dtype=jnp.int32) < count
    rows_input = jnp.where(valid[:, None], stream[index], jnp.zeros((), jnp.bfloat16))
    rows_grad = (weight[index][:, None] * out_cotangent[index].astype(jnp.float32))
    rows_grad = jnp.where(valid[:, None], rows_grad, 0.0).astype(jnp.bfloat16)
    gate = jnp.dot(rows_input, w_gate, preferred_element_type=jnp.float32)
    up = jnp.dot(rows_input, w_up, preferred_element_type=jnp.float32)
    sig = jax.nn.sigmoid(gate)
    silu_gate = gate * sig
    hidden = (silu_gate * up).astype(jnp.bfloat16)
    d_hidden = lax.dot_general(rows_grad, w_down, (((1,), (1,)), ((), ())), preferred_element_type=jnp.float32)
    d_gate = (d_hidden * up * sig * (1.0 + gate * (1.0 - sig))).astype(jnp.bfloat16)
    d_up = (d_hidden * silu_gate).astype(jnp.bfloat16)
    over_rows = (((0,), (0,)), ((), ()))
    grad_down = lax.dot_general(hidden, rows_grad, over_rows, preferred_element_type=jnp.float32).astype(jnp.bfloat16)
    grad_gate = lax.dot_general(rows_input, d_gate, over_rows, preferred_element_type=jnp.float32).astype(jnp.bfloat16)
    grad_up = lax.dot_general(rows_input, d_up, over_rows, preferred_element_type=jnp.float32).astype(jnp.bfloat16)
    block = FF // N_TP
    gate_blocks = d_gate.astype(jnp.float32).reshape(SLOTS, N_TP, block)
    up_blocks = d_up.astype(jnp.float32).reshape(SLOTS, N_TP, block)
    wg_blocks = w_gate.astype(jnp.float32).reshape(D, N_TP, block)
    wu_blocks = w_up.astype(jnp.float32).reshape(D, N_TP, block)
    partials = jnp.einsum('snf,dnf->nsd', gate_blocks, wg_blocks) + jnp.einsum('snf,dnf->nsd', up_blocks, wu_blocks)
    partials = partials.astype(jnp.bfloat16).astype(jnp.float32)
    row_grad = jnp.sum(partials, axis=0).astype(jnp.bfloat16)
    row_grad = jnp.where(valid[:, None], row_grad.astype(jnp.float32), 0.0)
    return index, row_grad, grad_gate, grad_up, grad_down


def reference(out_cotangent, stream, route_ids, route_weights, gate_proj, up_proj, down_proj,
              outer_gate, inner_gate, conv_input, conv_taps, out_proj):
    def step(carry, inputs):
        w_gate, w_up, w_down, expert = inputs
        index, row_grad, grad_gate, grad_up, grad_down = expert_backward(
            out_cotangent, stream, route_ids, route_weights, w_gate, w_up, w_down, expert)
        carry = carry.at[index].add(row_grad)
        return carry, (grad_gate, grad_up, grad_down)

    moe_grad, grads = lax.scan(step, jnp.zeros((TOKENS, D), jnp.float32),
                               (gate_proj, up_proj, down_proj, jnp.arange(EXPERTS, dtype=jnp.int32)))
    grad_gate_proj, grad_up_proj, grad_down_proj = grads
    stream_grad = (out_cotangent.astype(jnp.float32) + moe_grad).astype(jnp.bfloat16)
    mixed = inner_gate.astype(jnp.float32) * conv_input.astype(jnp.float32)
    padded = jnp.concatenate([jnp.zeros((2, CONV), jnp.float32), mixed], axis=0)
    conv_out = conv_taps[0] * padded[:TOKENS] + conv_taps[1] * padded[1:TOKENS + 1] + conv_taps[2] * padded[2:]
    mixer_out = (outer_gate.astype(jnp.float32) * conv_out).astype(jnp.bfloat16)
    d_mixer = jnp.dot(stream_grad, out_proj, preferred_element_type=jnp.float32)
    grad_outer_gate = d_mixer * conv_out
    d_conv = d_mixer * outer_gate.astype(jnp.float32)
    trailing = jnp.concatenate([d_conv, jnp.zeros((2, CONV), jnp.float32)], axis=0)
    d_mixed = conv_taps[2] * trailing[:TOKENS] + conv_taps[1] * trailing[1:TOKENS + 1] + conv_taps[0] * trailing[2:]
    grad_inner_gate = d_mixed * conv_input.astype(jnp.float32)
    grad_conv_input = d_mixed * inner_gate.astype(jnp.float32)
    grad_out_proj = lax.dot_general(stream_grad, mixer_out, (((0,), (0,)), ((), ())), preferred_element_type=jnp.float32)
    return (grad_gate_proj, grad_up_proj, grad_down_proj, grad_out_proj,
            grad_outer_gate, grad_inner_gate, grad_conv_input)
```

```python
import functools

import jax
import jax.numpy as jnp
from jax import lax
from jax.experimental import pallas as pl
from jax.experimental.pallas import tpu as pltpu
from jax.sharding import PartitionSpec as P

F32 = jnp.float32
BF16 = jnp.bfloat16
OVER_ROWS = (((0,), (0,)), ((), ()))
ACROSS = (((1,), (1,)), ((), ()))


def dot(a, b, dims=(((1,), (0,)), ((), ()))):
    return lax.dot_general(a, b, dims, preferred_element_type=F32)


def whole(shape):
    return pl.BlockSpec(shape, lambda *_: (0,) * len(shape))


def cost(flops, bytes_accessed):
    return pl.CostEstimate(flops=flops, bytes_accessed=bytes_accessed, transcendentals=0)


def route_kernel(capacity, block, tp_ref, ids_ref, x_ref, dest_ref, out_ref):
    step = pl.program_id(0)
    tokens = ids_ref.shape[1]

    @pl.when(step == 0)
    def _():
        experts = out_ref.shape[0] * pl.num_programs(0) // capacity
        first, second = ids_ref[0:1, :], ids_ref[1:2, :]
        names = lax.broadcasted_iota(jnp.int32, (experts, tokens), 0)
        one = jnp.where(names == first, 1.0, 0.0)
        two = jnp.where(names == second, 1.0, 0.0)
        before = jnp.where(
            lax.broadcasted_iota(jnp.int32, (tokens, tokens), 0)
            < lax.broadcasted_iota(jnp.int32, (tokens, tokens), 1),
            1.0,
            0.0,
        ).astype(BF16)
        count_one = dot(one.astype(BF16), before)
        count_two = dot(two.astype(BF16), before) + jnp.sum(one, axis=1, keepdims=True)
        rank_one = jnp.sum(one * count_one, axis=0, keepdims=True).astype(jnp.int32)
        rank_two = jnp.sum(two * count_two, axis=0, keepdims=True).astype(jnp.int32)
        dest_ref[0:1, :] = first * capacity + rank_one
        dest_ref[1:2, :] = second * capacity + rank_two

    slots = lax.broadcasted_iota(jnp.int32, (block, tokens), 0) + step * block
    hit = (slots == dest_ref[0:1, :]) | (slots == dest_ref[1:2, :])
    out_ref[...] = dot(jnp.where(hit, 1.0, 0.0).astype(BF16), x_ref[...]).astype(BF16)


def scale_kernel(block, tp_ref, dest_ref, w_ref, x_ref, out_ref):
    tokens = dest_ref.shape[1]
    slots = lax.broadcasted_iota(jnp.int32, (block, tokens), 0) + pl.program_id(0) * block
    one = jnp.where(slots == dest_ref[0:1, :], 1.0, 0.0)
    two = jnp.where(slots == dest_ref[1:2, :], 1.0, 0.0)
    weight = jnp.sum(one * w_ref[0:1, :] + two * w_ref[1:2, :], axis=1, keepdims=True)
    rows = dot((one + two).astype(BF16), x_ref[...])
    out_ref[...] = (rows * weight).astype(BF16)


def quarter(tp, by, n):
    return lax.rem(tp + by, n)


def up_kernel(n, tp_ref, own, right, opp, left, wg_ref, wu_ref, gate_ref, up_ref, full_ref):
    tp = tp_ref[0]
    width = own.shape[1]
    gate = up = None
    for by, piece in enumerate((own, right, opp, left)):
        start = pl.multiple_of(quarter(tp, by, n) * width, width)
        x = piece[...]
        full_ref[:, pl.ds(start, width)] = x
        g = dot(x, wg_ref[pl.ds(start, width), :])
        u = dot(x, wu_ref[pl.ds(start, width), :])
        gate = g if gate is None else gate + g
        up = u if up is None else up + u
    gate_ref[...] = gate
    up_ref[...] = up


def down_kernel(
    n, tp_ref, own, right, opp, left, gate_ref, up_ref, wd_ref, wg_ref, wu_ref,
    hidden_ref, dgate_ref, dup_ref, own_out, right_out, opp_out, left_out, full_ref,
):
    tp = tp_ref[0]
    width = own.shape[1]
    d_hidden = None
    for by, piece in enumerate((own, right, opp, left)):
        start = pl.multiple_of(quarter(tp, by, n) * width, width)
        x = piece[...]
        full_ref[:, pl.ds(start, width)] = x
        d = dot(x, wd_ref[:, pl.ds(start, width)], ACROSS)
        d_hidden = d if d_hidden is None else d_hidden + d
    gate, up = gate_ref[...], up_ref[...]
    sig = jax.nn.sigmoid(gate)
    silu = gate * sig
    hidden_ref[...] = (silu * up).astype(BF16)
    d_gate = (d_hidden * up * sig * (1.0 + gate * (1.0 - sig))).astype(BF16)
    d_up = (d_hidden * silu).astype(BF16)
    dgate_ref[...] = d_gate
    dup_ref[...] = d_up
    for by, out in enumerate((own_out, right_out, opp_out, left_out)):
        start = pl.multiple_of(quarter(tp, by, n) * width, width)
        rows = dot(d_gate, wg_ref[pl.ds(start, width), :], ACROSS)
        rows = rows + dot(d_up, wu_ref[pl.ds(start, width), :], ACROSS)
        out[...] = rows.astype(BF16)


def sum_kernel(a0, a1, a2, b0, b1, b2, out_ref):
    out_ref[0] = (a0[...].astype(F32) + a1[...].astype(F32) + a2[...].astype(F32)).astype(BF16)
    out_ref[1] = (b0[...].astype(F32) + b1[...].astype(F32) + b2[...].astype(F32)).astype(BF16)


def token_kernel(
    n, tp_ref, dest_ref, back_ref, cot_ref, proj_ref, m_own, m_right, m_opp, m_left,
    mix_ref, grad_ref,
):
    tp = tp_ref[0]
    tokens = dest_ref.shape[1]
    slots = lax.broadcasted_iota(jnp.int32, (back_ref.shape[0], tokens), 0)
    hit = (slots == dest_ref[0:1, :]) | (slots == dest_ref[1:2, :])
    moe = dot(jnp.where(hit, 1.0, 0.0).astype(BF16), back_ref[...], OVER_ROWS)
    part = (cot_ref[...].astype(F32) + moe).astype(BF16)
    for block in range(n):
        mix_ref[block] = dot(part, proj_ref[block])
    for by, piece in enumerate((m_own, m_right, m_opp, m_left)):
        g = dot(part, piece[...], OVER_ROWS).astype(BF16)
        grad_ref[:, quarter(tp, by, n)] = g.reshape(grad_ref.shape[0], *grad_ref.shape[2:])


def shards(
    out_cotangent,
    stream,
    route_ids,
    route_weights,
    gate_proj,
    up_proj,
    down_proj,
    outer_gate,
    inner_gate,
    conv_input,
    conv_taps,
    out_proj,
):
    sp_devices = lax.axis_size("sp")
    n = lax.axis_size("tp")
    tp = lax.axis_index("tp").astype(jnp.int32)[None]
    tokens, width = stream.shape
    experts = sp_devices * gate_proj.shape[0]
    capacity = 4 * tokens // experts
    slots = experts * capacity
    q = width // n
    hidden_units = gate_proj.shape[2]
    channels = out_proj.shape[1]
    ahead = [(i, (i + 1) % n) for i in range(n)]
    back = [(i, (i - 1) % n) for i in range(n)]

    def to_right(x):
        return lax.ppermute(x, "tp", ahead)

    def to_left(x):
        return lax.ppermute(x, "tp", back)

    def over_sp(x):
        return lax.all_to_all(x, "sp", split_axis=0, concat_axis=0, tiled=True)

    ids = route_ids.T
    weights = route_weights.T
    block = 256
    steps = slots // block
    mine = pl.BlockSpec((tokens, q), lambda i, t: (0, t[0]))
    dest, send_x = pl.pallas_call(
        functools.partial(route_kernel, capacity, block),
        grid_spec=pltpu.PrefetchScalarGridSpec(
            num_scalar_prefetch=1,
            grid=(steps,),
            in_specs=[whole((2, tokens)), mine],
            out_specs=[whole((2, tokens)), pl.BlockSpec((block, q), lambda i, t: (i, 0))],
        ),
        out_shape=[
            jax.ShapeDtypeStruct((2, tokens), jnp.int32),
            jax.ShapeDtypeStruct((slots, q), BF16),
        ],
        cost_estimate=cost(2 * slots * tokens * q, 2 * (slots + tokens) * q),
        name="route",
    )(tp, ids, stream)
    got_x = over_sp(send_x.reshape(sp_devices, -1, q)).reshape(slots, q)
    send_c = pl.pallas_call(
        functools.partial(scale_kernel, block),
        grid_spec=pltpu.PrefetchScalarGridSpec(
            num_scalar_prefetch=1,
            grid=(steps,),
            in_specs=[whole((2, tokens)), whole((2, tokens)), mine],
            out_specs=pl.BlockSpec((block, q), lambda i, t: (i, 0)),
        ),
        out_shape=jax.ShapeDtypeStruct((slots, q), BF16),
        cost_estimate=cost(2 * slots * tokens * q, 2 * (slots + tokens) * q),
        name="scale",
    )(tp, dest, weights, out_cotangent)
    got_c = over_sp(send_c.reshape(sp_devices, -1, q)).reshape(slots, q)

    half = slots // 2

    def gathered(x):
        a, b = x[:half], x[half:]
        left_a, right_a = to_right(a), to_left(a)
        opp_a = to_right(left_a)
        right_b, left_b = to_left(b), to_right(b)
        opp_b = to_left(right_b)
        return (a, right_a, opp_a, left_a), (b, right_b, opp_b, left_b)

    w_gate, w_up, w_down = gate_proj[0], up_proj[0], down_proj[0]
    rows = 128
    piece = pl.BlockSpec((rows, q), lambda i, t: (i, 0))
    inner = pl.BlockSpec((rows, hidden_units), lambda i, t: (i, 0))
    wide = pl.BlockSpec((rows, width), lambda i, t: (i, 0))

    def expert_up(pieces):
        return pl.pallas_call(
            functools.partial(up_kernel, n),
            grid_spec=pltpu.PrefetchScalarGridSpec(
                num_scalar_prefetch=1,
                grid=(half // rows,),
                in_specs=[piece] * 4 + [whole(w_gate.shape)] * 2,
                out_specs=[inner, inner, wide],
            ),
            out_shape=[
                jax.ShapeDtypeStruct((half, hidden_units), F32),
                jax.ShapeDtypeStruct((half, hidden_units), F32),
                jax.ShapeDtypeStruct((half, width), BF16),
            ],
            cost_estimate=cost(4 * half * width * hidden_units, 4 * half * width),
            name="expert_up",
        )(tp, *pieces, w_gate, w_up)

    def expert_down(pieces, gate, up):
        return pl.pallas_call(
            functools.partial(down_kernel, n),
            grid_spec=pltpu.PrefetchScalarGridSpec(
                num_scalar_prefetch=1,
                grid=(half // rows,),
                in_specs=[piece] * 4
                + [inner] * 2
                + [whole(w_down.shape), whole(w_gate.shape), whole(w_up.shape)],
                out_specs=[inner] * 3 + [piece] * 4 + [wide],
            ),
            out_shape=[jax.ShapeDtypeStruct((half, hidden_units), BF16)] * 3
            + [jax.ShapeDtypeStruct((half, q), BF16)] * 4
            + [jax.ShapeDtypeStruct((half, width), BF16)],
            cost_estimate=cost(6 * half * width * hidden_units, 6 * half * width),
            name="expert_down",
        )(tp, *pieces, gate, up, w_down, w_gate, w_up)

    xa, xb = gathered(got_x)
    ca, cb = gathered(got_c)
    gate_a, up_a, x_a = expert_up(xa)
    gate_b, up_b, x_b = expert_up(xb)
    hid_a, dg_a, du_a, own_a, right_a, opp_a, left_a, c_a = expert_down(ca, gate_a, up_a)
    hid_b, dg_b, du_b, own_b, right_b, opp_b, left_b, c_b = expert_down(cb, gate_b, up_b)

    def added(x, y):
        return (x.astype(F32) + y.astype(F32)).astype(BF16)

    from_opp_a = to_right(opp_a)
    one_a = to_left(left_a)
    two_a = to_right(added(right_a, from_opp_a))
    from_opp_b = to_left(opp_b)
    one_b = to_right(right_b)
    two_b = to_left(added(left_b, from_opp_b))
    part = pl.BlockSpec((rows, q), lambda i: (i, 0))
    share = pl.pallas_call(
        sum_kernel,
        grid=(half // rows,),
        in_specs=[part] * 6,
        out_specs=pl.BlockSpec((2, rows, q), lambda i: (0, i, 0)),
        out_shape=jax.ShapeDtypeStruct((2, half, q), BF16),
        cost_estimate=cost(4 * slots * q, 8 * slots * q),
        name="share",
    )(own_a, one_a, two_a, own_b, one_b, two_b)
    returned = over_sp(share.reshape(sp_devices, -1, q)).reshape(slots, q)

    grad_gate = (dot(x_a, dg_a, OVER_ROWS) + dot(x_b, dg_b, OVER_ROWS)).astype(BF16)
    grad_up = (dot(x_a, du_a, OVER_ROWS) + dot(x_b, du_b, OVER_ROWS)).astype(BF16)
    grad_down = (dot(hid_a, c_a, OVER_ROWS) + dot(hid_b, c_b, OVER_ROWS)).astype(BF16)

    mixed = inner_gate.astype(F32) * conv_input.astype(F32)
    sp_ahead = [(i, i + 1) for i in range(sp_devices - 1)]
    sp_back = [(i + 1, i) for i in range(sp_devices - 1)]
    previous = lax.ppermute(mixed[tokens - 2 :], "sp", sp_ahead)
    extended = jnp.concatenate([previous, mixed], axis=0)
    conv_out = (
        conv_taps[0] * extended[:tokens]
        + conv_taps[1] * extended[1 : tokens + 1]
        + conv_taps[2] * extended[2:]
    )
    mixer_out = (outer_gate.astype(F32) * conv_out).astype(BF16)
    mixer_left = to_right(mixer_out)
    mixer_right = to_left(mixer_out)
    mixer_opp = to_right(mixer_left)
    proj_rows = lax.all_to_all(out_proj.reshape(n, q, channels), "tp", 0, 0, tiled=True)

    strip = width // sp_devices
    row_blocks = q // strip
    partial_mix, partial_grad = pl.pallas_call(
        functools.partial(token_kernel, n),
        grid_spec=pltpu.PrefetchScalarGridSpec(
            num_scalar_prefetch=1,
            grid=(1,),
            in_specs=[
                whole((2, tokens)),
                whole((slots, q)),
                mine,
                whole((n, q, channels)),
            ]
            + [whole((tokens, channels))] * 4,
            out_specs=[whole((n, tokens, channels)), whole((row_blocks, n, strip, channels))],
        ),
        out_shape=[
            jax.ShapeDtypeStruct((n, tokens, channels), F32),
            jax.ShapeDtypeStruct((row_blocks, n, strip, channels), BF16),
        ],
        cost_estimate=cost(2 * slots * tokens * q + 16 * tokens * q * channels, 4 * slots * q),
        name="token",
    )(
        tp, dest, returned, out_cotangent, proj_rows,
        mixer_out, mixer_right, mixer_opp, mixer_left,
    )
    summed = over_sp(partial_grad.reshape(sp_devices, strip, channels)).astype(F32).sum(axis=0)
    home = [
        (s * n + t, (row_blocks * t + s // n) * n + s % n)
        for s in range(sp_devices)
        for t in range(n)
    ]
    grad_projection = lax.ppermute(summed, ("sp", "tp"), home)

    d_mixer = lax.all_to_all(partial_mix, "tp", 0, 0, tiled=True).sum(axis=0)
    grad_outer = d_mixer * conv_out
    d_conv = d_mixer * outer_gate.astype(F32)
    following = lax.ppermute(d_conv[:2], "sp", sp_back)
    trailing = jnp.concatenate([d_conv, following], axis=0)
    d_mixed = (
        conv_taps[2] * trailing[:tokens]
        + conv_taps[1] * trailing[1 : tokens + 1]
        + conv_taps[0] * trailing[2:]
    )
    grad_inner = d_mixed * conv_input.astype(F32)
    grad_input = d_mixed * inner_gate.astype(F32)
    return (
        grad_gate[None],
        grad_up[None],
        grad_down[None],
        grad_projection,
        grad_outer,
        grad_inner,
        grad_input,
    )


def solution(mesh):
    placed = (
        P("sp", None),
        P("sp", None),
        P("sp", None),
        P("sp", None),
        P("sp", None, "tp"),
        P("sp", None, "tp"),
        P("sp", "tp", None),
        P("sp", "tp"),
        P("sp", "tp"),
        P("sp", "tp"),
        P(None, "tp"),
        P(None, "tp"),
    )
    return jax.shard_map(
        shards,
        mesh=mesh,
        in_specs=placed,
        out_specs=(
            P("sp", None, "tp"),
            P("sp", None, "tp"),
            P("sp", "tp", None),
            P("sp", "tp"),
            P("sp", "tp"),
            P("sp", "tp"),
            P("sp", "tp"),
        ),
        check_vma=False,
    )
```

```python
import functools

import jax
import jax.numpy as jnp
from jax import lax
from jax.experimental import pallas as pl
from jax.experimental.pallas import tpu as pltpu
from jax.sharding import PartitionSpec as P


F32 = jnp.float32
BF16 = jnp.bfloat16
OVER_ROWS = (((0,), (0,)), ((), ()))
ACROSS = (((1,), (1,)), ((), ()))


def dot(a, b, dims=(((1,), (0,)), ((), ()))):
    return lax.dot_general(a, b, dims, preferred_element_type=F32)


def whole(shape):
    return pl.BlockSpec(shape, lambda *_: (0,) * len(shape))


def cost(flops, bytes_accessed):
    return pl.CostEstimate(flops=flops, bytes_accessed=bytes_accessed, transcendentals=0)


def find_slots(capacity, experts, ids_ref, dest_ref):
    tokens = ids_ref.shape[1]
    first, second = ids_ref[0:1, :], ids_ref[1:2, :]
    names = lax.broadcasted_iota(jnp.int32, (experts, tokens), 0)
    one = jnp.where(names == first, 1.0, 0.0)
    two = jnp.where(names == second, 1.0, 0.0)
    before = jnp.where(
        lax.broadcasted_iota(jnp.int32, (tokens, tokens), 0)
        < lax.broadcasted_iota(jnp.int32, (tokens, tokens), 1),
        1.0,
        0.0,
    ).astype(BF16)
    count_one = dot(one.astype(BF16), before)
    count_two = dot(two.astype(BF16), before) + jnp.sum(one, axis=1, keepdims=True)
    rank_one = jnp.sum(one * count_one, axis=0, keepdims=True).astype(jnp.int32)
    rank_two = jnp.sum(two * count_two, axis=0, keepdims=True).astype(jnp.int32)
    dest_ref[0:1, :] = first * capacity + rank_one
    dest_ref[1:2, :] = second * capacity + rank_two


def half_slots(rows, tokens, capacity, which):
    cut = capacity // 2
    index = lax.broadcasted_iota(jnp.int32, (rows, tokens), 0)
    return (index // cut) * capacity + lax.rem(index, cut) + which * cut


def fill_half(capacity, which, dest_ref, w_ref, x_ref, c_ref, out_ref):
    experts, cut = out_ref.shape[0], capacity // 2
    tokens, width = x_ref.shape
    slots = half_slots(experts * cut, tokens, capacity, which)
    one = jnp.where(slots == dest_ref[0:1, :], 1.0, 0.0)
    two = jnp.where(slots == dest_ref[1:2, :], 1.0, 0.0)
    hit = (one + two).astype(BF16)
    out_ref[:, 0] = dot(hit, x_ref[...]).reshape(experts, cut, width).astype(BF16)
    weight = jnp.sum(one * w_ref[0:1, :] + two * w_ref[1:2, :], axis=1, keepdims=True)
    rows = dot(hit, c_ref[...]) * weight
    out_ref[:, 1] = rows.reshape(experts, cut, width).astype(BF16)


def route_kernel(capacity, tp_ref, ids_ref, w_ref, x_ref, c_ref, dest_ref, out_ref):
    find_slots(capacity, out_ref.shape[0], ids_ref, dest_ref)
    fill_half(capacity, 0, dest_ref, w_ref, x_ref, c_ref, out_ref)


def rest_kernel(capacity, tp_ref, dest_ref, w_ref, x_ref, c_ref, out_ref):
    fill_half(capacity, 1, dest_ref, w_ref, x_ref, c_ref, out_ref)


def quarter(tp, by, n):
    return lax.rem(tp + by, n)


def up_kernel(n, tp_ref, own, right, opp, left, wg_ref, wu_ref, gate_ref, up_ref):
    tp = tp_ref[0]
    width = own.shape[1]
    gate = up = None
    for by, piece in enumerate((own, right, opp, left)):
        start = pl.multiple_of(quarter(tp, by, n) * width, width)
        x = piece[...]
        g = dot(x, wg_ref[pl.ds(start, width), :])
        u = dot(x, wu_ref[pl.ds(start, width), :])
        gate = g if gate is None else gate + g
        up = u if up is None else up + u
    gate_ref[...] = gate
    up_ref[...] = up


def down_kernel(
    n, tp_ref, own, right, opp, left, gate_ref, up_ref, wd_ref, wg_ref, wu_ref,
    hidden_ref, dgate_ref, dup_ref, own_out, right_out, opp_out, left_out,
):
    tp = tp_ref[0]
    width = own.shape[1]
    d_hidden = None
    for by, piece in enumerate((own, right, opp, left)):
        start = pl.multiple_of(quarter(tp, by, n) * width, width)
        d = dot(piece[...], wd_ref[:, pl.ds(start, width)], ACROSS)
        d_hidden = d if d_hidden is None else d_hidden + d
    gate, up = gate_ref[...], up_ref[...]
    sig = jax.nn.sigmoid(gate)
    silu = gate * sig
    hidden_ref[...] = (silu * up).astype(BF16)
    d_gate = (d_hidden * up * sig * (1.0 + gate * (1.0 - sig))).astype(BF16)
    d_up = (d_hidden * silu).astype(BF16)
    dgate_ref[...] = d_gate
    dup_ref[...] = d_up
    for by, out in enumerate((own_out, right_out, opp_out, left_out)):
        start = pl.multiple_of(quarter(tp, by, n) * width, width)
        rows = dot(d_gate, wg_ref[pl.ds(start, width), :], ACROSS)
        rows = rows + dot(d_up, wu_ref[pl.ds(start, width), :], ACROSS)
        out[...] = rows.astype(BF16)


def assemble_kernel(n, tp_ref, *refs):
    x_full, c_full, hidden, d_gate, d_up = refs[-5:]
    tp = tp_ref[0]
    width = refs[0].shape[1]
    for half in range(2):
        for by in range(n):
            start = pl.multiple_of(quarter(tp, by, n) * width, width)
            x_full[half, :, pl.ds(start, width)] = refs[n * half + by][...]
            c_full[half, :, pl.ds(start, width)] = refs[n * (2 + half) + by][...]
        for place, out in enumerate((hidden, d_gate, d_up)):
            out[half] = refs[4 * n + 3 * half + place][...]


def token_kernel(
    n, tp_ref, dest_ref, back_ref, cot_ref, p_own, p_right, p_opp, p_left,
    m_own, m_right, m_opp, m_left,
    grad_ref, mix_own, mix_right, mix_opp, mix_left,
):
    tp = tp_ref[0]
    tokens = dest_ref.shape[1]
    at = lax.broadcasted_iota(jnp.int32, (back_ref.shape[0], tokens), 0)
    hit = (at == dest_ref[0:1, :]) | (at == dest_ref[1:2, :])
    terms = dot(jnp.where(hit, 1.0, 0.0).astype(BF16), back_ref[...], OVER_ROWS)
    part = (cot_ref[...].astype(F32) + terms).astype(BF16)
    for by, piece in enumerate((m_own, m_right, m_opp, m_left)):
        g = dot(part, piece[...], OVER_ROWS).astype(BF16)
        grad_ref[:, quarter(tp, by, n)] = g.reshape(grad_ref.shape[0], *grad_ref.shape[2:])
    for piece, out in ((p_own, mix_own), (p_right, mix_right), (p_opp, mix_opp), (p_left, mix_left)):
        out[...] = dot(part, piece[...])


def shards(
    out_cotangent,
    stream,
    route_ids,
    route_weights,
    gate_proj,
    up_proj,
    down_proj,
    outer_gate,
    inner_gate,
    conv_input,
    conv_taps,
    out_proj,
):
    sp_devices = lax.axis_size("sp")
    n = lax.axis_size("tp")
    tp = lax.axis_index("tp").astype(jnp.int32)[None]
    tokens, width = stream.shape
    experts = sp_devices * gate_proj.shape[0]
    capacity = 4 * tokens // experts
    slots = experts * capacity
    q = width // n
    hidden_units = gate_proj.shape[2]
    channels = out_proj.shape[1]
    ahead = [(i, (i + 1) % n) for i in range(n)]
    back = [(i, (i - 1) % n) for i in range(n)]

    def to_right(x):
        return lax.ppermute(x, "tp", ahead)

    def to_left(x):
        return lax.ppermute(x, "tp", back)

    def over_sp(x):
        return lax.all_to_all(x, "sp", split_axis=0, concat_axis=0, tiled=True)

    ids = route_ids.T
    weights = route_weights.T
    cut = capacity // 2
    half = slots // 2
    mine = pl.BlockSpec((tokens, q), lambda i, t: (0, t[0]))
    pair = whole((2, tokens))
    packed = jax.ShapeDtypeStruct((experts, 2, cut, q), BF16)
    fill_cost = cost(4 * half * tokens * q, 8 * tokens * q)
    dest, send_a = pl.pallas_call(
        functools.partial(route_kernel, capacity),
        grid_spec=pltpu.PrefetchScalarGridSpec(
            num_scalar_prefetch=1,
            grid=(1,),
            in_specs=[pair, pair, mine, mine],
            out_specs=[pair, whole(packed.shape)],
        ),
        out_shape=[jax.ShapeDtypeStruct((2, tokens), jnp.int32), packed],
        cost_estimate=fill_cost,
        name="route",
    )(tp, ids, weights, stream, out_cotangent)
    send_b = pl.pallas_call(
        functools.partial(rest_kernel, capacity),
        grid_spec=pltpu.PrefetchScalarGridSpec(
            num_scalar_prefetch=1,
            grid=(1,),
            in_specs=[pair, pair, mine, mine],
            out_specs=whole(packed.shape),
        ),
        out_shape=packed,
        cost_estimate=fill_cost,
        name="rest",
    )(tp, dest, weights, stream, out_cotangent)
    got_a = over_sp(send_a.reshape(sp_devices, 2 * cut, q))
    got_b = over_sp(send_b.reshape(sp_devices, 2 * cut, q))

    def gathered(got):
        x = got[:, :cut].reshape(half, q)
        c = got[:, cut:].reshape(half, q)
        x_left = to_right(x)
        c_right = to_left(c)
        c_left = to_right(c)
        x_right = to_left(x)
        x_opp = to_right(x_left)
        c_opp = to_left(c_right)
        return (x, x_right, x_opp, x_left), (c, c_right, c_opp, c_left)

    w_gate, w_up, w_down = gate_proj[0], up_proj[0], down_proj[0]
    rows = 256
    piece = pl.BlockSpec((rows, q), lambda i, t: (i, 0))
    inner = pl.BlockSpec((rows, hidden_units), lambda i, t: (i, 0))

    def expert_up(pieces):
        return pl.pallas_call(
            functools.partial(up_kernel, n),
            grid_spec=pltpu.PrefetchScalarGridSpec(
                num_scalar_prefetch=1,
                grid=(half // rows,),
                in_specs=[piece] * 4 + [whole(w_gate.shape)] * 2,
                out_specs=[inner, inner],
            ),
            out_shape=[jax.ShapeDtypeStruct((half, hidden_units), F32)] * 2,
            cost_estimate=cost(4 * half * width * hidden_units, 4 * half * width),
            compiler_params=pltpu.CompilerParams(vmem_limit_bytes=20 << 20),
            name="expert_up",
        )(tp, *pieces, w_gate, w_up)

    def expert_down(pieces, gate, up):
        return pl.pallas_call(
            functools.partial(down_kernel, n),
            grid_spec=pltpu.PrefetchScalarGridSpec(
                num_scalar_prefetch=1,
                grid=(half // rows,),
                in_specs=[piece] * 4
                + [inner] * 2
                + [whole(w_down.shape), whole(w_gate.shape), whole(w_up.shape)],
                out_specs=[inner] * 3 + [piece] * 4,
            ),
            out_shape=[jax.ShapeDtypeStruct((half, hidden_units), BF16)] * 3
            + [jax.ShapeDtypeStruct((half, q), BF16)] * 4,
            cost_estimate=cost(6 * half * width * hidden_units, 6 * half * width),
            compiler_params=pltpu.CompilerParams(vmem_limit_bytes=30 << 20),
            name="expert_down",
        )(tp, *pieces, gate, up, w_down, w_gate, w_up)

    xa, ca = gathered(got_a)
    xb, cb = gathered(got_b)
    gate_a, up_a = expert_up(xa)
    gate_b, up_b = expert_up(xb)
    *inner_a, own_a, right_a, opp_a, left_a = expert_down(ca, gate_a, up_a)
    *inner_b, own_b, right_b, opp_b, left_b = expert_down(cb, gate_b, up_b)

    def added(*terms):
        total = terms[0].astype(F32)
        for term in terms[1:]:
            total = total + term.astype(F32)
        return total.astype(BF16)

    from_opp_a = to_right(opp_a)
    one_a = to_left(left_a)
    two_a = to_right(added(right_a, from_opp_a))
    from_opp_b = to_left(opp_b)
    one_b = to_right(right_b)
    two_b = to_left(added(left_b, from_opp_b))

    def returned_rows(own, one, two):
        return added(own, one, two).reshape(sp_devices, 1, cut, q)

    share = jnp.concatenate(
        [returned_rows(own_a, one_a, two_a), returned_rows(own_b, one_b, two_b)], axis=1
    )
    back_rows = over_sp(share.reshape(sp_devices, capacity, q)).reshape(slots, q)

    strips = 64
    piece = pl.BlockSpec((strips, q), lambda i, t: (i, 0))
    inner = pl.BlockSpec((strips, hidden_units), lambda i, t: (i, 0))
    outs = [(2, half, width)] * 2 + [(2, half, hidden_units)] * 3
    full = pl.pallas_call(
        functools.partial(assemble_kernel, n),
        grid_spec=pltpu.PrefetchScalarGridSpec(
            num_scalar_prefetch=1,
            grid=(half // strips,),
            in_specs=[piece] * (4 * n) + [inner] * 6,
            out_specs=[
                pl.BlockSpec((2, strips, shape[2]), lambda i, t: (0, i, 0)) for shape in outs
            ],
        ),
        out_shape=[jax.ShapeDtypeStruct(shape, BF16) for shape in outs],
        cost_estimate=cost(64 * slots * width, 8 * slots * width),
        name="assemble",
    )(tp, *xa, *xb, *ca, *cb, *inner_a, *inner_b)
    x_full, c_full, hidden, d_gate, d_up = [y.reshape(slots, y.shape[2]) for y in full]
    grad_gate = dot(x_full, d_gate, OVER_ROWS).astype(BF16)
    grad_up = dot(x_full, d_up, OVER_ROWS).astype(BF16)
    grad_down = dot(hidden, c_full, OVER_ROWS).astype(BF16)

    strip = width // sp_devices
    row_blocks = q // strip
    opposite = [(i, (i + 2) % n) for i in range(n)]

    def to_opposite(x):
        return lax.ppermute(x, "tp", opposite)

    mixed = inner_gate.astype(F32) * conv_input.astype(F32)
    sp_ahead = [(i, i + 1) for i in range(sp_devices - 1)]
    sp_back = [(i + 1, i) for i in range(sp_devices - 1)]
    previous = lax.ppermute(mixed[tokens - 2 :], "sp", sp_ahead)
    extended = jnp.concatenate([previous, mixed], axis=0)
    conv_out = (
        conv_taps[0] * extended[:tokens]
        + conv_taps[1] * extended[1 : tokens + 1]
        + conv_taps[2] * extended[2:]
    )
    mixer_out = (outer_gate.astype(F32) * conv_out).astype(BF16)
    mixer_left = to_right(mixer_out)
    mixer_right = to_left(mixer_out)
    mixer_opp = to_opposite(mixer_out)

    def block_of(by):
        return lax.dynamic_slice_in_dim(out_proj, lax.rem(tp[0] + by, n) * q, q, 0)

    proj_own = block_of(0)
    proj_left = to_right(block_of(1))
    proj_right = to_left(block_of(n - 1))
    proj_opp = to_opposite(block_of(2))

    partial_grad, mix_own, mix_right, mix_opp, mix_left = pl.pallas_call(
        functools.partial(token_kernel, n),
        grid_spec=pltpu.PrefetchScalarGridSpec(
            num_scalar_prefetch=1,
            grid=(1,),
            in_specs=[pair, whole((slots, q)), mine]
            + [whole((q, channels))] * 4
            + [whole((tokens, channels))] * 4,
            out_specs=[whole((row_blocks, n, strip, channels))] + [whole((tokens, channels))] * 4,
        ),
        out_shape=[jax.ShapeDtypeStruct((row_blocks, n, strip, channels), BF16)]
        + [jax.ShapeDtypeStruct((tokens, channels), F32)] * 4,
        cost_estimate=cost(2 * slots * tokens * q + 16 * tokens * q * channels, 4 * slots * q),
        compiler_params=pltpu.CompilerParams(vmem_limit_bytes=24 << 20),
        name="token",
    )(
        tp, dest, back_rows, out_cotangent,
        proj_own, proj_right, proj_opp, proj_left,
        mixer_out, mixer_right, mixer_opp, mixer_left,
    )
    pieces = over_sp(partial_grad.reshape(sp_devices, strip, channels))
    summed = pieces.astype(F32).sum(axis=0)
    home = [
        (s * n + t, (row_blocks * t + s // n) * n + s % n)
        for s in range(sp_devices)
        for t in range(n)
    ]
    grad_projection = lax.ppermute(summed, ("sp", "tp"), home)

    mix_from_left = to_right(mix_right)
    mix_from_right = to_left(mix_left)
    mix_from_opp = to_opposite(mix_opp)
    d_mixer = mix_own + mix_from_left + mix_from_right + mix_from_opp
    grad_outer = d_mixer * conv_out
    d_conv = d_mixer * outer_gate.astype(F32)
    following = lax.ppermute(d_conv[:2], "sp", sp_back)
    trailing = jnp.concatenate([d_conv, following], axis=0)
    d_mixed = (
        conv_taps[2] * trailing[:tokens]
        + conv_taps[1] * trailing[1 : tokens + 1]
        + conv_taps[0] * trailing[2:]
    )
    grad_inner = d_mixed * conv_input.astype(F32)
    grad_input = d_mixed * inner_gate.astype(F32)
    return (
        grad_gate[None],
        grad_up[None],
        grad_down[None],
        grad_projection,
        grad_outer,
        grad_inner,
        grad_input,
    )


def solution(mesh):
    placed = (
        P("sp", None),
        P("sp", None),
        P("sp", None),
        P("sp", None),
        P("sp", None, "tp"),
        P("sp", None, "tp"),
        P("sp", "tp", None),
        P("sp", "tp"),
        P("sp", "tp"),
        P("sp", "tp"),
        P(None, "tp"),
        P(None, "tp"),
    )
    return jax.shard_map(
        shards,
        mesh=mesh,
        in_specs=placed,
        out_specs=(
            P("sp", None, "tp"),
            P("sp", None, "tp"),
            P("sp", "tp", None),
            P("sp", "tp"),
            P("sp", "tp"),
            P("sp", "tp"),
            P("sp", "tp"),
        ),
        check_vma=False,
    )
```

```python
import functools

import jax
import jax.numpy as jnp
from jax import lax
from jax.experimental import pallas as pl
from jax.experimental.pallas import tpu as pltpu
from jax.sharding import PartitionSpec as P


F32 = jnp.float32
BF16 = jnp.bfloat16
OVER_ROWS = (((0,), (0,)), ((), ()))
ACROSS = (((1,), (1,)), ((), ()))


def dot(a, b, dims=(((1,), (0,)), ((), ()))):
    return lax.dot_general(a, b, dims, preferred_element_type=F32)


def whole(shape):
    return pl.BlockSpec(shape, lambda *_: (0,) * len(shape))


def cost(flops, bytes_accessed):
    return pl.CostEstimate(flops=flops, bytes_accessed=bytes_accessed, transcendentals=0)


def find_slots(capacity, experts, ids_ref, dest_ref):
    tokens = ids_ref.shape[1]
    first, second = ids_ref[0:1, :], ids_ref[1:2, :]
    names = lax.broadcasted_iota(jnp.int32, (experts, tokens), 0)
    one = jnp.where(names == first, 1.0, 0.0)
    two = jnp.where(names == second, 1.0, 0.0)
    before = jnp.where(
        lax.broadcasted_iota(jnp.int32, (tokens, tokens), 0)
        < lax.broadcasted_iota(jnp.int32, (tokens, tokens), 1),
        1.0,
        0.0,
    ).astype(BF16)
    count_one = dot(one.astype(BF16), before)
    count_two = dot(two.astype(BF16), before) + jnp.sum(one, axis=1, keepdims=True)
    rank_one = jnp.sum(one * count_one, axis=0, keepdims=True).astype(jnp.int32)
    rank_two = jnp.sum(two * count_two, axis=0, keepdims=True).astype(jnp.int32)
    dest_ref[0:1, :] = first * capacity + rank_one
    dest_ref[1:2, :] = second * capacity + rank_two


def half_slots(rows, tokens, capacity, which):
    cut = capacity // 2
    index = lax.broadcasted_iota(jnp.int32, (rows, tokens), 0)
    return (index // cut) * capacity + lax.rem(index, cut) + which * cut


def fill_half(capacity, which, dest_ref, w_ref, x_ref, c_ref, out_ref):
    experts, cut = out_ref.shape[0], capacity // 2
    tokens, width = x_ref.shape
    slots = half_slots(experts * cut, tokens, capacity, which)
    one = jnp.where(slots == dest_ref[0:1, :], 1.0, 0.0)
    two = jnp.where(slots == dest_ref[1:2, :], 1.0, 0.0)
    hit = (one + two).astype(BF16)
    out_ref[:, 0] = dot(hit, x_ref[...]).reshape(experts, cut, width).astype(BF16)
    weight = jnp.sum(one * w_ref[0:1, :] + two * w_ref[1:2, :], axis=1, keepdims=True)
    rows = dot(hit, c_ref[...]) * weight
    out_ref[:, 1] = rows.reshape(experts, cut, width).astype(BF16)


def route_kernel(capacity, tp_ref, ids_ref, w_ref, x_ref, c_ref, dest_ref, out_ref):
    find_slots(capacity, out_ref.shape[0], ids_ref, dest_ref)
    fill_half(capacity, 0, dest_ref, w_ref, x_ref, c_ref, out_ref)


def rest_kernel(capacity, tp_ref, dest_ref, w_ref, x_ref, c_ref, out_ref):
    fill_half(capacity, 1, dest_ref, w_ref, x_ref, c_ref, out_ref)


def quarter(tp, by, n):
    return lax.rem(tp + by, n)


def up_kernel(n, tp_ref, own, right, opp, left, wg_ref, wu_ref, gate_ref, up_ref):
    tp = tp_ref[0]
    width = own.shape[1]
    gate = up = None
    for by, piece in enumerate((own, right, opp, left)):
        start = pl.multiple_of(quarter(tp, by, n) * width, width)
        x = piece[...]
        g = dot(x, wg_ref[pl.ds(start, width), :])
        u = dot(x, wu_ref[pl.ds(start, width), :])
        gate = g if gate is None else gate + g
        up = u if up is None else up + u
    gate_ref[...] = gate
    up_ref[...] = up


def activations(n, tp, pieces, gate_ref, up_ref, wd_ref, hidden_ref, dgate_ref, dup_ref):
    width = pieces[0].shape[1]
    d_hidden = None
    for by, piece in enumerate(pieces):
        start = pl.multiple_of(quarter(tp, by, n) * width, width)
        d = dot(piece[...], wd_ref[:, pl.ds(start, width)], ACROSS)
        d_hidden = d if d_hidden is None else d_hidden + d
    gate, up = gate_ref[...], up_ref[...]
    sig = jax.nn.sigmoid(gate)
    silu = gate * sig
    hidden_ref[0] = (silu * up).astype(BF16)
    d_gate = (d_hidden * up * sig * (1.0 + gate * (1.0 - sig))).astype(BF16)
    d_up = (d_hidden * silu).astype(BF16)
    dgate_ref[0] = d_gate
    dup_ref[0] = d_up
    return d_gate, d_up


def down_kernel(
    n, tp_ref, own, right, opp, left, gate_ref, up_ref, wd_ref, wg_ref, wu_ref,
    first_hidden, first_dgate, first_dup,
    hidden_ref, dgate_ref, dup_ref, own_out, right_out, opp_out, left_out,
):
    tp = tp_ref[0]
    width = own.shape[1]
    d_gate, d_up = activations(
        n, tp, (own, right, opp, left), gate_ref, up_ref, wd_ref, hidden_ref, dgate_ref, dup_ref
    )
    for by, out in enumerate((own_out, right_out, opp_out, left_out)):
        start = pl.multiple_of(quarter(tp, by, n) * width, width)
        rows = dot(d_gate, wg_ref[pl.ds(start, width), :], ACROSS)
        rows = rows + dot(d_up, wu_ref[pl.ds(start, width), :], ACROSS)
        out[...] = rows.astype(BF16)


def down_whole_kernel(
    n, tp_ref, own, right, opp, left, gate_ref, up_ref, wd_ref, wg_ref, wu_ref,
    hidden_ref, dgate_ref, dup_ref, rows_ref,
):
    width = own.shape[1]
    d_gate, d_up = activations(
        n, tp_ref[0], (own, right, opp, left), gate_ref, up_ref, wd_ref,
        hidden_ref, dgate_ref, dup_ref,
    )
    for start in range(0, n * width, width):
        rows = dot(d_gate, wg_ref[start : start + width, :], ACROSS)
        rows = rows + dot(d_up, wu_ref[start : start + width, :], ACROSS)
        rows_ref[:, start : start + width] = rows.astype(BF16)


def assemble_kernel(n, tp_ref, *refs):
    x_full, c_full = refs[-2:]
    tp = tp_ref[0]
    width = refs[0].shape[1]
    for half in range(2):
        for by in range(n):
            start = pl.multiple_of(quarter(tp, by, n) * width, width)
            x_full[half, :, pl.ds(start, width)] = refs[n * half + by][...]
            c_full[half, :, pl.ds(start, width)] = refs[n * (2 + half) + by][...]


def chosen_slots(capacity, which, rows, dest_ref):
    at = half_slots(rows, dest_ref.shape[1], capacity, which)
    hit = (at == dest_ref[0:1, :]) | (at == dest_ref[1:2, :])
    return jnp.where(hit, 1.0, 0.0).astype(BF16)


def fold_kernel(n, capacity, tp_ref, dest_ref, back_ref, own, right, opp, left):
    tp = tp_ref[0]
    width = own.shape[1]
    hit = chosen_slots(capacity, 0, back_ref.shape[0], dest_ref)
    for by, out in enumerate((own, right, opp, left)):
        start = pl.multiple_of(quarter(tp, by, n) * width, width)
        terms = dot(hit, back_ref[:, pl.ds(start, width)], OVER_ROWS)
        out[...] = terms.astype(out.dtype)


def token_kernel(
    capacity, tp_ref, dest_ref, back_ref, cot_ref, own, one, two, three,
    p_own, p_right, p_opp, p_left, m_own, m_right, m_opp, m_left, *outs,
):
    hit = chosen_slots(capacity, 1, back_ref.shape[0], dest_ref)
    terms = dot(hit, back_ref[...], OVER_ROWS) + own[...]
    for other in (one, two, three):
        terms = terms + other[...].astype(F32)
    part = (cot_ref[...].astype(F32) + terms).astype(BF16)
    width = part.shape[1]
    projs, mixers = (p_own, p_right, p_opp, p_left), (m_own, m_right, m_opp, m_left)
    for proj, mixer, out in zip(projs, mixers, outs):
        out[:width, :] = dot(part, mixer[...], OVER_ROWS).astype(BF16)
        out[width:, :] = dot(part, proj[...]).astype(BF16)


def place_kernel(n, tp_ref, own, right, opp, left, grad_ref, mix_ref):
    width = grad_ref.shape[1]
    total = None
    for by, piece in enumerate((own, right, opp, left)):
        grad_ref[quarter(tp_ref[0], by, n)] = piece[:width, :]
        mix = piece[width:, :].astype(F32)
        total = mix if total is None else total + mix
    mix_ref[...] = total


def shards(
    out_cotangent,
    stream,
    route_ids,
    route_weights,
    gate_proj,
    up_proj,
    down_proj,
    outer_gate,
    inner_gate,
    conv_input,
    conv_taps,
    out_proj,
):
    sp_devices = lax.axis_size("sp")
    n = lax.axis_size("tp")
    tp = lax.axis_index("tp").astype(jnp.int32)[None]
    tokens, width = stream.shape
    experts = sp_devices * gate_proj.shape[0]
    capacity = 4 * tokens // experts
    slots = experts * capacity
    q = width // n
    hidden_units = gate_proj.shape[2]
    channels = out_proj.shape[1]
    ahead = [(i, (i + 1) % n) for i in range(n)]
    back = [(i, (i - 1) % n) for i in range(n)]

    def to_right(x):
        return lax.ppermute(x, "tp", ahead)

    def to_left(x):
        return lax.ppermute(x, "tp", back)

    def over_sp(x):
        return lax.all_to_all(x, "sp", split_axis=0, concat_axis=0, tiled=True)

    ids = route_ids.T
    weights = route_weights.T
    cut = capacity // 2
    half = slots // 2
    mine = pl.BlockSpec((tokens, q), lambda i, t: (0, t[0]))
    pair = whole((2, tokens))
    packed = jax.ShapeDtypeStruct((experts, 2, cut, q), BF16)
    fill_cost = cost(4 * half * tokens * q, 8 * tokens * q)
    dest, send_a = pl.pallas_call(
        functools.partial(route_kernel, capacity),
        grid_spec=pltpu.PrefetchScalarGridSpec(
            num_scalar_prefetch=1,
            grid=(1,),
            in_specs=[pair, pair, mine, mine],
            out_specs=[pair, whole(packed.shape)],
        ),
        out_shape=[jax.ShapeDtypeStruct((2, tokens), jnp.int32), packed],
        cost_estimate=fill_cost,
        name="route",
    )(tp, ids, weights, stream, out_cotangent)
    send_b = pl.pallas_call(
        functools.partial(rest_kernel, capacity),
        grid_spec=pltpu.PrefetchScalarGridSpec(
            num_scalar_prefetch=1,
            grid=(1,),
            in_specs=[pair, pair, mine, mine],
            out_specs=whole(packed.shape),
        ),
        out_shape=packed,
        cost_estimate=fill_cost,
        name="rest",
    )(tp, dest, weights, stream, out_cotangent)
    got_a = over_sp(send_a.reshape(sp_devices, 2 * cut, q))
    got_b = over_sp(send_b.reshape(sp_devices, 2 * cut, q))

    def gathered(got):
        x = got[:, :cut].reshape(half, q)
        c = got[:, cut:].reshape(half, q)
        x_left = to_right(x)
        c_right = to_left(c)
        c_left = to_right(c)
        x_right = to_left(x)
        x_opp = to_right(x_left)
        c_opp = to_left(c_right)
        return (x, x_right, x_opp, x_left), (c, c_right, c_opp, c_left)

    w_gate, w_up, w_down = gate_proj[0], up_proj[0], down_proj[0]
    rows = 256
    piece = pl.BlockSpec((rows, q), lambda i, t: (i, 0))
    inner = pl.BlockSpec((rows, hidden_units), lambda i, t: (i, 0))

    def expert_up(pieces):
        return pl.pallas_call(
            functools.partial(up_kernel, n),
            grid_spec=pltpu.PrefetchScalarGridSpec(
                num_scalar_prefetch=1,
                grid=(half // rows,),
                in_specs=[piece] * 4 + [whole(w_gate.shape)] * 2,
                out_specs=[inner, inner],
            ),
            out_shape=[jax.ShapeDtypeStruct((half, hidden_units), F32)] * 2,
            cost_estimate=cost(4 * half * width * hidden_units, 4 * half * width),
            compiler_params=pltpu.CompilerParams(vmem_limit_bytes=20 << 20),
            name="expert_up",
        )(tp, *pieces, w_gate, w_up)

    def expert_down(kernel, which, out_specs, out_shape, pieces, gate, up, first):
        kept = pl.BlockSpec((1, rows, hidden_units), lambda i, t: (which, i, 0))
        return pl.pallas_call(
            functools.partial(kernel, n),
            grid_spec=pltpu.PrefetchScalarGridSpec(
                num_scalar_prefetch=1,
                grid=(half // rows,),
                in_specs=[piece] * 4
                + [inner] * 2
                + [whole(w_down.shape), whole(w_gate.shape), whole(w_up.shape)]
                + [pl.BlockSpec(memory_space=pl.ANY)] * len(first),
                out_specs=[kept] * 3 + out_specs,
            ),
            out_shape=[pltpu.HBM((2, half, hidden_units), BF16)] * 3 + out_shape,
            input_output_aliases={10 + i: i for i in range(len(first))},
            cost_estimate=cost(6 * half * width * hidden_units, 6 * half * width),
            compiler_params=pltpu.CompilerParams(vmem_limit_bytes=30 << 20),
            name="expert_down",
        )(tp, *pieces, gate, up, w_down, w_gate, w_up, *first)

    xa, ca = gathered(got_a)
    xb, cb = gathered(got_b)
    gate_a, up_a = expert_up(xa)
    gate_b, up_b = expert_up(xb)
    *inner_a, rows_a = expert_down(
        down_whole_kernel,
        0,
        [pl.BlockSpec((rows, width), lambda i, t: (i, 0))],
        [pltpu.HBM((half, width), BF16)],
        ca, gate_a, up_a, (),
    )
    *inners, own_b, right_b, opp_b, left_b = expert_down(
        down_kernel, 1, [piece] * 4, [jax.ShapeDtypeStruct((half, q), BF16)] * 4,
        cb, gate_b, up_b, inner_a,
    )

    back_a = over_sp(rows_a.reshape(sp_devices, cut, width)).reshape(half, width)

    def added(*terms):
        total = terms[0].astype(F32)
        for term in terms[1:]:
            total = total + term.astype(F32)
        return total.astype(BF16)

    opposite = [(i, (i + 2) % n) for i in range(n)]

    def to_opposite(x):
        return lax.ppermute(x, "tp", opposite)

    def exchanged(right, opp, left):
        from_left = to_right(right)
        from_right = to_left(left)
        from_opp = to_opposite(opp)
        return from_right, from_opp, from_left

    from_opp_b = to_left(opp_b)
    one_b = to_right(right_b)
    two_b = to_left(added(left_b, from_opp_b))
    share_b = added(own_b, one_b, two_b)
    back_b = over_sp(share_b.reshape(sp_devices, cut, q)).reshape(half, q)
    fold_own, *fold_rest = pl.pallas_call(
        functools.partial(fold_kernel, n, capacity),
        grid_spec=pltpu.PrefetchScalarGridSpec(
            num_scalar_prefetch=1,
            grid=(1,),
            in_specs=[pair, whole((half, width))],
            out_specs=[whole((tokens, q))] * 4,
        ),
        out_shape=[jax.ShapeDtypeStruct((tokens, q), F32)]
        + [jax.ShapeDtypeStruct((tokens, q), BF16)] * 3,
        cost_estimate=cost(2 * half * tokens * width, 2 * half * width),
        compiler_params=pltpu.CompilerParams(vmem_limit_bytes=24 << 20),
        name="fold",
    )(tp, dest, back_a)
    fold_others = exchanged(*fold_rest)

    strips = 64
    piece = pl.BlockSpec((strips, q), lambda i, t: (i, 0))
    outs = [(2, half, width)] * 2
    full = pl.pallas_call(
        functools.partial(assemble_kernel, n),
        grid_spec=pltpu.PrefetchScalarGridSpec(
            num_scalar_prefetch=1,
            grid=(half // strips,),
            in_specs=[piece] * (4 * n),
            out_specs=[
                pl.BlockSpec((2, strips, shape[2]), lambda i, t: (0, i, 0)) for shape in outs
            ],
        ),
        out_shape=[pltpu.HBM(shape, BF16) for shape in outs],
        cost_estimate=cost(64 * slots * width, 8 * slots * width),
        compiler_params=pltpu.CompilerParams(vmem_limit_bytes=20 << 20),
        name="assemble",
    )(tp, *xa, *xb, *ca, *cb)
    x_full, c_full = [y.reshape(slots, width) for y in full]
    hidden, d_gate, d_up = [y.reshape(slots, hidden_units) for y in inners]
    grad_gate = dot(x_full, d_gate, OVER_ROWS).astype(BF16)
    grad_up = dot(x_full, d_up, OVER_ROWS).astype(BF16)
    grad_down = dot(hidden, c_full, OVER_ROWS).astype(BF16)

    strip = width // sp_devices
    mixed = inner_gate.astype(F32) * conv_input.astype(F32)
    sp_ahead = [(i, i + 1) for i in range(sp_devices - 1)]
    sp_back = [(i + 1, i) for i in range(sp_devices - 1)]
    previous = lax.ppermute(mixed[tokens - 2 :], "sp", sp_ahead)
    extended = jnp.concatenate([previous, mixed], axis=0)
    conv_out = (
        conv_taps[0] * extended[:tokens]
        + conv_taps[1] * extended[1 : tokens + 1]
        + conv_taps[2] * extended[2:]
    )
    mixer_out = (outer_gate.astype(F32) * conv_out).astype(BF16)
    mixer_left = to_right(mixer_out)
    mixer_right = to_left(mixer_out)
    mixer_opp = to_opposite(mixer_out)

    def block_of(by):
        return lax.dynamic_slice_in_dim(out_proj, lax.rem(tp[0] + by, n) * q, q, 0)

    proj_own = block_of(0)
    proj_left = to_right(block_of(1))
    proj_right = to_left(block_of(n - 1))
    proj_opp = to_opposite(block_of(2))

    packed_block = (q + tokens, channels)
    own_block, *other_blocks = pl.pallas_call(
        functools.partial(token_kernel, capacity),
        grid_spec=pltpu.PrefetchScalarGridSpec(
            num_scalar_prefetch=1,
            grid=(1,),
            in_specs=[pair, whole((half, q)), mine]
            + [whole((tokens, q))] * 4
            + [whole((q, channels))] * 4
            + [whole((tokens, channels))] * 4,
            out_specs=[whole(packed_block)] * n,
        ),
        out_shape=[jax.ShapeDtypeStruct(packed_block, BF16)] * n,
        cost_estimate=cost(2 * slots * tokens * q + 16 * tokens * q * channels, 4 * slots * q),
        compiler_params=pltpu.CompilerParams(vmem_limit_bytes=24 << 20),
        name="token",
    )(
        tp, dest, back_b, out_cotangent, fold_own, *fold_others,
        proj_own, proj_right, proj_opp, proj_left,
        mixer_out, mixer_right, mixer_opp, mixer_left,
    )
    other_blocks = exchanged(*other_blocks)
    partial_grad, d_mixer = pl.pallas_call(
        functools.partial(place_kernel, n),
        grid_spec=pltpu.PrefetchScalarGridSpec(
            num_scalar_prefetch=1,
            grid=(1,),
            in_specs=[whole(packed_block)] * 4,
            out_specs=[whole((n, q, channels)), whole((tokens, channels))],
        ),
        out_shape=[
            pltpu.HBM((n, q, channels), BF16),
            jax.ShapeDtypeStruct((tokens, channels), F32),
        ],
        cost_estimate=cost(4 * tokens * channels, 4 * width * channels),
        compiler_params=pltpu.CompilerParams(vmem_limit_bytes=24 << 20),
        name="place",
    )(tp, own_block, *other_blocks)
    pieces = over_sp(partial_grad.reshape(sp_devices, strip, channels))
    grad_projection = pieces.astype(F32).sum(axis=0)

    grad_outer = d_mixer * conv_out
    d_conv = d_mixer * outer_gate.astype(F32)
    following = lax.ppermute(d_conv[:2], "sp", sp_back)
    trailing = jnp.concatenate([d_conv, following], axis=0)
    d_mixed = (
        conv_taps[2] * trailing[:tokens]
        + conv_taps[1] * trailing[1 : tokens + 1]
        + conv_taps[0] * trailing[2:]
    )
    grad_inner = d_mixed * conv_input.astype(F32)
    grad_input = d_mixed * inner_gate.astype(F32)
    return (
        grad_gate[None],
        grad_up[None],
        grad_down[None],
        grad_projection,
        grad_outer,
        grad_inner,
        grad_input,
    )


def solution(mesh):
    placed = (
        P("sp", None),
        P("sp", None),
        P("sp", None),
        P("sp", None),
        P("sp", None, "tp"),
        P("sp", None, "tp"),
        P("sp", "tp", None),
        P("sp", "tp"),
        P("sp", "tp"),
        P("sp", "tp"),
        P(None, "tp"),
        P(None, "tp"),
    )
    return jax.shard_map(
        shards,
        mesh=mesh,
        in_specs=placed,
        out_specs=(
            P("sp", None, "tp"),
            P("sp", None, "tp"),
            P("sp", "tp", None),
            P("sp", "tp"),
            P("sp", "tp"),
            P("sp", "tp"),
            P("sp", "tp"),
        ),
        check_vma=False,
    )
```

```python
import functools

import jax
import jax.numpy as jnp
from jax import lax
from jax.experimental import pallas as pl
from jax.experimental.pallas import tpu as pltpu
from jax.sharding import PartitionSpec as P


F32 = jnp.float32
BF16 = jnp.bfloat16
OVER_ROWS = (((0,), (0,)), ((), ()))
ACROSS = (((1,), (1,)), ((), ()))


def dot(a, b, dims=(((1,), (0,)), ((), ()))):
    return lax.dot_general(a, b, dims, preferred_element_type=F32)


def whole(shape):
    return pl.BlockSpec(shape, lambda *_: (0,) * len(shape))


def cost(flops, bytes_accessed):
    return pl.CostEstimate(flops=flops, bytes_accessed=bytes_accessed, transcendentals=0)


def find_slots(capacity, experts, ids_ref, dest_ref):
    tokens = ids_ref.shape[1]
    first, second = ids_ref[0:1, :], ids_ref[1:2, :]
    names = lax.broadcasted_iota(jnp.int32, (experts, tokens), 0)
    one = jnp.where(names == first, 1.0, 0.0)
    two = jnp.where(names == second, 1.0, 0.0)
    before = jnp.where(
        lax.broadcasted_iota(jnp.int32, (tokens, tokens), 0)
        < lax.broadcasted_iota(jnp.int32, (tokens, tokens), 1),
        1.0,
        0.0,
    ).astype(BF16)
    count_one = dot(one.astype(BF16), before)
    count_two = dot(two.astype(BF16), before) + jnp.sum(one, axis=1, keepdims=True)
    rank_one = jnp.sum(one * count_one, axis=0, keepdims=True).astype(jnp.int32)
    rank_two = jnp.sum(two * count_two, axis=0, keepdims=True).astype(jnp.int32)
    dest_ref[0:1, :] = first * capacity + rank_one
    dest_ref[1:2, :] = second * capacity + rank_two


def half_slots(rows, tokens, capacity, which):
    cut = capacity // 2
    index = lax.broadcasted_iota(jnp.int32, (rows, tokens), 0)
    return (index // cut) * capacity + lax.rem(index, cut) + which * cut


def fill_half(capacity, which, dest_ref, w_ref, x_ref, c_ref, out_ref):
    experts, cut = out_ref.shape[0], capacity // 2
    tokens, width = x_ref.shape
    slots = half_slots(experts * cut, tokens, capacity, which)
    one = jnp.where(slots == dest_ref[0:1, :], 1.0, 0.0)
    two = jnp.where(slots == dest_ref[1:2, :], 1.0, 0.0)
    hit = (one + two).astype(BF16)
    out_ref[:, 0] = dot(hit, x_ref[...]).reshape(experts, cut, width).astype(BF16)
    weight = jnp.sum(one * w_ref[0:1, :] + two * w_ref[1:2, :], axis=1, keepdims=True)
    rows = dot(hit, c_ref[...]) * weight
    out_ref[:, 1] = rows.reshape(experts, cut, width).astype(BF16)


def route_kernel(capacity, tp_ref, ids_ref, w_ref, x_ref, c_ref, dest_ref, out_ref):
    find_slots(capacity, out_ref.shape[0], ids_ref, dest_ref)
    fill_half(capacity, 0, dest_ref, w_ref, x_ref, c_ref, out_ref)


def rest_kernel(capacity, tp_ref, dest_ref, w_ref, x_ref, c_ref, out_ref):
    fill_half(capacity, 1, dest_ref, w_ref, x_ref, c_ref, out_ref)


def quarter(tp, by, n):
    return lax.rem(tp + by, n)


def up_kernel(n, tp_ref, own, right, opp, left, wg_ref, wu_ref, gate_ref, up_ref):
    tp = tp_ref[0]
    width = own.shape[1]
    gate = up = None
    for by, piece in enumerate((own, right, opp, left)):
        start = pl.multiple_of(quarter(tp, by, n) * width, width)
        x = piece[...]
        g = dot(x, wg_ref[pl.ds(start, width), :])
        u = dot(x, wu_ref[pl.ds(start, width), :])
        gate = g if gate is None else gate + g
        up = u if up is None else up + u
    gate_ref[...] = gate
    up_ref[...] = up


def activations(n, tp, pieces, gate_ref, up_ref, wd_ref, hidden_ref, dgate_ref, dup_ref):
    width = pieces[0].shape[1]
    d_hidden = None
    for by, piece in enumerate(pieces):
        start = pl.multiple_of(quarter(tp, by, n) * width, width)
        d = dot(piece[...], wd_ref[:, pl.ds(start, width)], ACROSS)
        d_hidden = d if d_hidden is None else d_hidden + d
    gate, up = gate_ref[...], up_ref[...]
    sig = jax.nn.sigmoid(gate)
    silu = gate * sig
    hidden_ref[0] = (silu * up).astype(BF16)
    d_gate = (d_hidden * up * sig * (1.0 + gate * (1.0 - sig))).astype(BF16)
    d_up = (d_hidden * silu).astype(BF16)
    dgate_ref[0] = d_gate
    dup_ref[0] = d_up
    return d_gate, d_up


def down_kernel(
    n, tp_ref, own, right, opp, left, gate_ref, up_ref, wd_ref, wg_ref, wu_ref,
    first_hidden, first_dgate, first_dup,
    hidden_ref, dgate_ref, dup_ref, own_out, *parts,
):
    tp = tp_ref[0]
    step = pl.program_id(0)
    width = own.shape[1]
    d_gate, d_up = activations(
        n, tp, (own, right, opp, left), gate_ref, up_ref, wd_ref, hidden_ref, dgate_ref, dup_ref
    )
    for by in range(n):
        start = pl.multiple_of(quarter(tp, by, n) * width, width)
        rows = dot(d_gate, wg_ref[pl.ds(start, width), :], ACROSS)
        rows = (rows + dot(d_up, wu_ref[pl.ds(start, width), :], ACROSS)).astype(BF16)
        if by == 0:
            own_out[...] = rows
            continue
        for place in range(2):

            @pl.when(step == place)
            def _(rows=rows, out=parts[2 * by - 2 + place]):
                out[...] = rows


def share_kernel(own, top_one, top_two, bot_one, bot_two, out_ref):
    rows = top_one.shape[0]
    for start, one, two in ((0, top_one, top_two), (rows, bot_one, bot_two)):
        total = own[start : start + rows, :].astype(F32) + one[...].astype(F32)
        out_ref[start : start + rows, :] = (total + two[...].astype(F32)).astype(BF16)


def down_whole_kernel(
    n, tp_ref, own, right, opp, left, gate_ref, up_ref, wd_ref, wg_ref, wu_ref,
    hidden_ref, dgate_ref, dup_ref, rows_ref,
):
    width = own.shape[1]
    d_gate, d_up = activations(
        n, tp_ref[0], (own, right, opp, left), gate_ref, up_ref, wd_ref,
        hidden_ref, dgate_ref, dup_ref,
    )
    for start in range(0, n * width, width):
        rows = dot(d_gate, wg_ref[start : start + width, :], ACROSS)
        rows = rows + dot(d_up, wu_ref[start : start + width, :], ACROSS)
        rows_ref[:, start : start + width] = rows.astype(BF16)


def assemble_kernel(n, tp_ref, *refs):
    x_full, c_full = refs[-2:]
    tp = tp_ref[0]
    width = refs[0].shape[1]
    for half in range(2):
        for by in range(n):
            start = pl.multiple_of(quarter(tp, by, n) * width, width)
            x_full[half, :, pl.ds(start, width)] = refs[n * half + by][...]
            c_full[half, :, pl.ds(start, width)] = refs[n * (2 + half) + by][...]


def chosen_slots(capacity, which, rows, dest_ref):
    at = half_slots(rows, dest_ref.shape[1], capacity, which)
    hit = (at == dest_ref[0:1, :]) | (at == dest_ref[1:2, :])
    return jnp.where(hit, 1.0, 0.0).astype(BF16)


def fold_kernel(n, capacity, tp_ref, dest_ref, back_ref, own, right, opp, left):
    tp = tp_ref[0]
    width = own.shape[1]
    hit = chosen_slots(capacity, 0, back_ref.shape[0], dest_ref)
    for by, out in enumerate((own, right, opp, left)):
        start = pl.multiple_of(quarter(tp, by, n) * width, width)
        terms = dot(hit, back_ref[:, pl.ds(start, width)], OVER_ROWS)
        out[...] = terms.astype(out.dtype)


def token_kernel(
    capacity, tp_ref, dest_ref, back_ref, cot_ref, own, one, two, three,
    with_own, with_right, with_opp, with_left, *outs,
):
    hit = chosen_slots(capacity, 1, back_ref.shape[0], dest_ref)
    terms = dot(hit, back_ref[...], OVER_ROWS) + own[...]
    for other in (one, two, three):
        terms = terms + other[...].astype(F32)
    part = (cot_ref[...].astype(F32) + terms).astype(BF16)
    width = part.shape[1]
    for pack, out in zip((with_own, with_right, with_opp, with_left), outs):
        out[:width, :] = dot(part, pack[width:, :], OVER_ROWS).astype(BF16)
        out[width:, :] = dot(part, pack[:width, :]).astype(BF16)


def place_kernel(n, tp_ref, own, right, opp, left, grad_ref, mix_ref):
    width = grad_ref.shape[1]
    total = None
    for by, piece in enumerate((own, right, opp, left)):
        grad_ref[quarter(tp_ref[0], by, n)] = piece[:width, :]
        mix = piece[width:, :].astype(F32)
        total = mix if total is None else total + mix
    mix_ref[...] = total


def shards(
    out_cotangent,
    stream,
    route_ids,
    route_weights,
    gate_proj,
    up_proj,
    down_proj,
    outer_gate,
    inner_gate,
    conv_input,
    conv_taps,
    out_proj,
):
    sp_devices = lax.axis_size("sp")
    n = lax.axis_size("tp")
    tp = lax.axis_index("tp").astype(jnp.int32)[None]
    tokens, width = stream.shape
    experts = sp_devices * gate_proj.shape[0]
    capacity = 4 * tokens // experts
    slots = experts * capacity
    q = width // n
    hidden_units = gate_proj.shape[2]
    channels = out_proj.shape[1]
    ahead = [(i, (i + 1) % n) for i in range(n)]
    back = [(i, (i - 1) % n) for i in range(n)]

    def to_right(x):
        return lax.ppermute(x, "tp", ahead)

    def to_left(x):
        return lax.ppermute(x, "tp", back)

    def over_sp(x):
        return lax.all_to_all(x, "sp", split_axis=0, concat_axis=0, tiled=True)

    ids = route_ids.T
    weights = route_weights.T
    cut = capacity // 2
    half = slots // 2
    mine = pl.BlockSpec((tokens, q), lambda i, t: (0, t[0]))
    pair = whole((2, tokens))
    packed = jax.ShapeDtypeStruct((experts, 2, cut, q), BF16)
    fill_cost = cost(4 * half * tokens * q, 8 * tokens * q)
    dest, send_a = pl.pallas_call(
        functools.partial(route_kernel, capacity),
        grid_spec=pltpu.PrefetchScalarGridSpec(
            num_scalar_prefetch=1,
            grid=(1,),
            in_specs=[pair, pair, mine, mine],
            out_specs=[pair, whole(packed.shape)],
        ),
        out_shape=[jax.ShapeDtypeStruct((2, tokens), jnp.int32), packed],
        cost_estimate=fill_cost,
        name="route",
    )(tp, ids, weights, stream, out_cotangent)
    send_b = pl.pallas_call(
        functools.partial(rest_kernel, capacity),
        grid_spec=pltpu.PrefetchScalarGridSpec(
            num_scalar_prefetch=1,
            grid=(1,),
            in_specs=[pair, pair, mine, mine],
            out_specs=whole(packed.shape),
        ),
        out_shape=packed,
        cost_estimate=fill_cost,
        name="rest",
    )(tp, dest, weights, stream, out_cotangent)
    got_a = over_sp(send_a.reshape(sp_devices, 2 * cut, q))
    got_b = over_sp(send_b.reshape(sp_devices, 2 * cut, q))

    def gathered(got):
        x = got[:, :cut].reshape(half, q)
        c = got[:, cut:].reshape(half, q)
        x_left = to_right(x)
        c_right = to_left(c)
        c_left = to_right(c)
        x_right = to_left(x)
        x_opp = to_right(x_left)
        c_opp = to_left(c_right)
        return (x, x_right, x_opp, x_left), (c, c_right, c_opp, c_left)

    w_gate, w_up, w_down = gate_proj[0], up_proj[0], down_proj[0]
    rows = 256
    piece = pl.BlockSpec((rows, q), lambda i, t: (i, 0))
    inner = pl.BlockSpec((rows, hidden_units), lambda i, t: (i, 0))

    def expert_up(pieces):
        return pl.pallas_call(
            functools.partial(up_kernel, n),
            grid_spec=pltpu.PrefetchScalarGridSpec(
                num_scalar_prefetch=1,
                grid=(half // rows,),
                in_specs=[piece] * 4 + [whole(w_gate.shape)] * 2,
                out_specs=[inner, inner],
            ),
            out_shape=[jax.ShapeDtypeStruct((half, hidden_units), F32)] * 2,
            cost_estimate=cost(4 * half * width * hidden_units, 4 * half * width),
            compiler_params=pltpu.CompilerParams(vmem_limit_bytes=20 << 20),
            name="expert_up",
        )(tp, *pieces, w_gate, w_up)

    def expert_down(kernel, which, out_specs, out_shape, pieces, gate, up, first):
        kept = pl.BlockSpec((1, rows, hidden_units), lambda i, t: (which, i, 0))
        return pl.pallas_call(
            functools.partial(kernel, n),
            grid_spec=pltpu.PrefetchScalarGridSpec(
                num_scalar_prefetch=1,
                grid=(half // rows,),
                in_specs=[piece] * 4
                + [inner] * 2
                + [whole(w_down.shape), whole(w_gate.shape), whole(w_up.shape)]
                + [pl.BlockSpec(memory_space=pl.ANY)] * len(first),
                out_specs=[kept] * 3 + out_specs,
            ),
            out_shape=[pltpu.HBM((2, half, hidden_units), BF16)] * 3 + out_shape,
            input_output_aliases={10 + i: i for i in range(len(first))},
            cost_estimate=cost(6 * half * width * hidden_units, 6 * half * width),
            compiler_params=pltpu.CompilerParams(vmem_limit_bytes=30 << 20),
            name="expert_down",
        )(tp, *pieces, gate, up, w_down, w_gate, w_up, *first)

    xa, ca = gathered(got_a)
    xb, cb = gathered(got_b)
    gate_a, up_a = expert_up(xa)
    gate_b, up_b = expert_up(xb)
    *inner_a, rows_a = expert_down(
        down_whole_kernel,
        0,
        [pl.BlockSpec((rows, width), lambda i, t: (i, 0))],
        [pltpu.HBM((half, width), BF16)],
        ca, gate_a, up_a, (),
    )
    *inners, own_b, right_top, right_bot, opp_top, opp_bot, left_top, left_bot = expert_down(
        down_kernel,
        1,
        [piece] + [whole((rows, q))] * 6,
        [jax.ShapeDtypeStruct((half, q), BF16)] + [jax.ShapeDtypeStruct((rows, q), BF16)] * 6,
        cb, gate_b, up_b, inner_a,
    )

    back_a = over_sp(rows_a.reshape(sp_devices, cut, width)).reshape(half, width)

    def added(*terms):
        total = terms[0].astype(F32)
        for term in terms[1:]:
            total = total + term.astype(F32)
        return total.astype(BF16)

    opposite = [(i, (i + 2) % n) for i in range(n)]

    def to_opposite(x):
        return lax.ppermute(x, "tp", opposite)

    def exchanged(right, opp, left):
        from_left = to_right(right)
        from_right = to_left(left)
        from_opp = to_opposite(opp)
        return from_right, from_opp, from_left

    from_opp_top = to_right(opp_top)
    from_opp_bot = to_left(opp_bot)
    top_two = to_right(added(right_top, from_opp_top))
    bot_two = to_left(added(left_bot, from_opp_bot))
    bot_one = to_right(right_bot)
    top_one = to_left(left_top)
    share_b = pl.pallas_call(
        share_kernel,
        grid=(1,),
        in_specs=[whole((half, q))] + [whole((rows, q))] * 4,
        out_specs=whole((half, q)),
        out_shape=pltpu.HBM((half, q), BF16),
        cost_estimate=cost(3 * half * q, 8 * half * q),
        compiler_params=pltpu.CompilerParams(vmem_limit_bytes=16 << 20),
        name="share",
    )(own_b, top_one, top_two, bot_one, bot_two)
    back_b = over_sp(share_b.reshape(sp_devices, cut, q)).reshape(half, q)
    fold_own, *fold_rest = pl.pallas_call(
        functools.partial(fold_kernel, n, capacity),
        grid_spec=pltpu.PrefetchScalarGridSpec(
            num_scalar_prefetch=1,
            grid=(1,),
            in_specs=[pair, whole((half, width))],
            out_specs=[whole((tokens, q))] * 4,
        ),
        out_shape=[jax.ShapeDtypeStruct((tokens, q), F32)]
        + [jax.ShapeDtypeStruct((tokens, q), BF16)] * 3,
        cost_estimate=cost(2 * half * tokens * width, 2 * half * width),
        compiler_params=pltpu.CompilerParams(vmem_limit_bytes=24 << 20),
        name="fold",
    )(tp, dest, back_a)
    fold_others = exchanged(*fold_rest)

    strips = 64
    piece = pl.BlockSpec((strips, q), lambda i, t: (i, 0))
    outs = [(2, half, width)] * 2
    full = pl.pallas_call(
        functools.partial(assemble_kernel, n),
        grid_spec=pltpu.PrefetchScalarGridSpec(
            num_scalar_prefetch=1,
            grid=(half // strips,),
            in_specs=[piece] * (4 * n),
            out_specs=[
                pl.BlockSpec((2, strips, shape[2]), lambda i, t: (0, i, 0)) for shape in outs
            ],
        ),
        out_shape=[pltpu.HBM(shape, BF16) for shape in outs],
        cost_estimate=cost(64 * slots * width, 8 * slots * width),
        compiler_params=pltpu.CompilerParams(vmem_limit_bytes=20 << 20),
        name="assemble",
    )(tp, *xa, *xb, *ca, *cb)
    x_full, c_full = [y.reshape(slots, width) for y in full]
    hidden, d_gate, d_up = [y.reshape(slots, hidden_units) for y in inners]
    grad_gate = dot(x_full, d_gate, OVER_ROWS).astype(BF16)
    grad_up = dot(x_full, d_up, OVER_ROWS).astype(BF16)
    grad_down = dot(hidden, c_full, OVER_ROWS).astype(BF16)

    strip = width // sp_devices
    mixed = inner_gate.astype(F32) * conv_input.astype(F32)
    sp_ahead = [(i, i + 1) for i in range(sp_devices - 1)]
    sp_back = [(i + 1, i) for i in range(sp_devices - 1)]
    previous = lax.ppermute(mixed[tokens - 2 :], "sp", sp_ahead)
    extended = jnp.concatenate([previous, mixed], axis=0)
    conv_out = (
        conv_taps[0] * extended[:tokens]
        + conv_taps[1] * extended[1 : tokens + 1]
        + conv_taps[2] * extended[2:]
    )
    mixer_out = (outer_gate.astype(F32) * conv_out).astype(BF16)

    def pack_for(by):
        block = lax.dynamic_slice_in_dim(out_proj, lax.rem(tp[0] + by, n) * q, q, 0)
        return jnp.concatenate([block, mixer_out], axis=0)

    own_pack = pack_for(0)
    other_packs = exchanged(pack_for(1), pack_for(2), pack_for(n - 1))

    packed_block = (q + tokens, channels)
    own_block, *other_blocks = pl.pallas_call(
        functools.partial(token_kernel, capacity),
        grid_spec=pltpu.PrefetchScalarGridSpec(
            num_scalar_prefetch=1,
            grid=(1,),
            in_specs=[pair, whole((half, q)), mine]
            + [whole((tokens, q))] * 4
            + [whole(packed_block)] * 4,
            out_specs=[whole(packed_block)] * n,
        ),
        out_shape=[jax.ShapeDtypeStruct(packed_block, BF16)] * n,
        cost_estimate=cost(2 * slots * tokens * q + 16 * tokens * q * channels, 4 * slots * q),
        compiler_params=pltpu.CompilerParams(vmem_limit_bytes=24 << 20),
        name="token",
    )(
        tp, dest, back_b, out_cotangent, fold_own, *fold_others,
        own_pack, *other_packs,
    )
    other_blocks = exchanged(*other_blocks)
    partial_grad, d_mixer = pl.pallas_call(
        functools.partial(place_kernel, n),
        grid_spec=pltpu.PrefetchScalarGridSpec(
            num_scalar_prefetch=1,
            grid=(1,),
            in_specs=[whole(packed_block)] * 4,
            out_specs=[whole((n, q, channels)), whole((tokens, channels))],
        ),
        out_shape=[
            pltpu.HBM((n, q, channels), BF16),
            jax.ShapeDtypeStruct((tokens, channels), F32),
        ],
        cost_estimate=cost(4 * tokens * channels, 4 * width * channels),
        compiler_params=pltpu.CompilerParams(vmem_limit_bytes=24 << 20),
        name="place",
    )(tp, own_block, *other_blocks)
    pieces = over_sp(partial_grad.reshape(sp_devices, strip, channels))
    grad_projection = pieces.astype(F32).sum(axis=0)

    grad_outer = d_mixer * conv_out
    d_conv = d_mixer * outer_gate.astype(F32)
    following = lax.ppermute(d_conv[:2], "sp", sp_back)
    trailing = jnp.concatenate([d_conv, following], axis=0)
    d_mixed = (
        conv_taps[2] * trailing[:tokens]
        + conv_taps[1] * trailing[1 : tokens + 1]
        + conv_taps[0] * trailing[2:]
    )
    grad_inner = d_mixed * conv_input.astype(F32)
    grad_input = d_mixed * inner_gate.astype(F32)
    return (
        grad_gate[None],
        grad_up[None],
        grad_down[None],
        grad_projection,
        grad_outer,
        grad_inner,
        grad_input,
    )


def solution(mesh):
    placed = (
        P("sp", None),
        P("sp", None),
        P("sp", None),
        P("sp", None),
        P("sp", None, "tp"),
        P("sp", None, "tp"),
        P("sp", "tp", None),
        P("sp", "tp"),
        P("sp", "tp"),
        P("sp", "tp"),
        P(None, "tp"),
        P(None, "tp"),
    )
    return jax.shard_map(
        shards,
        mesh=mesh,
        in_specs=placed,
        out_specs=(
            P("sp", None, "tp"),
            P("sp", None, "tp"),
            P("sp", "tp", None),
            P("sp", "tp"),
            P("sp", "tp"),
            P("sp", "tp"),
            P("sp", "tp"),
        ),
        check_vma=False,
    )
```
